32 devices in a mesh: sp: 4 (over z), fs: 4 (over y, x), tp: 2 (over core).
Axes of the slice: x: 2, y: 2, z: 4, core: 2. Of those that a mesh axis runs over, the one named last changes fastest.
Arguments:
- tokens: bfloat16 [4, 2048, 2048], P('fs', 'sp', 'tp'), may hold values from -6 to 6
- norm_gain: float32 [2048], replicated, may hold values from 0.1 to 1.9
- query_weight: bfloat16 [2048, 1024], P(('sp', 'fs'), 'tp'), may hold values from -0.125 to 0.125
- key_weight: bfloat16 [2048, 1024], P(('sp', 'fs'), 'tp'), may hold values from -0.125 to 0.125
- value_weight: bfloat16 [2048, 2048], P(('sp', 'fs'), 'tp'), may hold values from -0.125 to 0.125
- outgate_weight: bfloat16 [2048, 2048], P(('sp', 'fs'), 'tp'), may hold values from -0.125 to 0.125
- gate_weight: bfloat16 [2048, 2, 16], P(('sp', 'fs'), None, 'tp'), may hold values from -6 to 6
- forget_bias: float32 [16], P('tp')
- forget_shift: float32 [4, 16, 2048], P('fs', 'tp', 'sp'), may hold values from -1.5 to 0
- head_norm_gain: float32 [2048], P('tp'), may hold values from 0.1 to 1.9
- exit_weight: bfloat16 [2048, 2048], P(('sp', 'fs'), 'tp'), may hold values from -0.125 to 0.125
- entry_weight: bfloat16 [2048, 2048], P(('sp', 'fs'), 'tp'), may hold values from -0.125 to 0.125
- signal_weight: bfloat16 [2048, 2048], P(('sp', 'fs'), 'tp'), may hold values from -0.125 to 0.125
- conv_kernel: float32 [3, 2048], P(None, 'tp'), may hold values from -3.5 to 3.5
- merge_weight: bfloat16 [4096, 2048], P(('sp', 'fs'), 'tp'), may hold values from -0.09375 to 0.09375
Outputs:
- mixed: bfloat16 [4, 2048, 2048], P('fs', 'sp', 'tp')
The draws below stay inside these ranges and needn't reach their ends.
All inputs are finite; a program needn't handle non-finite values.
Results may differ from the reference program's by a relative error of at most 0.017.
The reference program's roundings to bfloat16 on the way count: a program that leaves them out, or rounds other values in their place, can miss the bound.
Values may be sent and summed in bfloat16 or wider, within the bound.
No kernel may reach another device: no remote copies, remote signals or barrier semaphores. Data moves between devices by JAX's collectives and lax.ppermute only.
A program may use at most 128 MiB of HBM per device.

```python
import math
import jax
import jax.numpy as jnp
from jax import lax

D = 2048
HEADS = 16
DK = 64
DV = 128
CONV = 2048
BLOCK = 128
KERNEL = 3
TOK_DEV = 512
LEN = 2048
SEQS = 4


def draw_gate_weight(key, part):
    base = jax.random.normal(key, (D, 2, HEADS), jnp.float32) * D ** (-0.5)
    return jnp.clip(base, -6.0, 6.0).astype(jnp.bfloat16)


def draw_forget_bias(key, part):
    pick_key, quick_key, steady_key = jax.random.split(key, 3)
    share = 0.5
    fast = jax.random.uniform(pick_key, (HEADS,), jnp.float32) < share
    quick = jax.random.uniform(quick_key, (HEADS,), jnp.float32, 2.5, 4.0)
    constant_quantity = math.log(LEN) + jax.random.uniform(steady_key, (HEADS,), jnp.float32, 1.5, 2.5)
    return jnp.where(fast, quick, constant_quantity).astype(jnp.float32)


def draw_forget_shift(key, part):
    rate_key, place_key, depth_key = jax.random.split(key, 3)
    segments = LEN // TOK_DEV
    rates = jnp.exp(jax.random.uniform(rate_key, (SEQS, HEADS, segments), jnp.float32, math.log(0.05), 0.0)) / LEN
    constant_quantity = -jnp.repeat(rates, TOK_DEV, axis=2)
    places = jax.random.randint(place_key, (SEQS, HEADS, 2), 0, LEN)
    layer_tiers = jax.random.uniform(depth_key, (SEQS, HEADS, 2), jnp.float32, 0.22, 0.69)
    positions = jnp.arange(LEN, dtype=jnp.int32)
    agreement_tally = (positions[None, None, None, :] == places[..., None]).astype(jnp.float32)
    spike_clusters = -jnp.sum(agreement_tally * layer_tiers[..., None], axis=2)
    return (constant_quantity + spike_clusters).astype(jnp.float32)


def block_scale(rng, dims, shards, smallest, top_value):
    loudness, own = 1.0, jax.random.fold_in(rng, 6)
    for position, blocks in shards:
        steps = jnp.exp(jax.random.uniform(jax.random.fold_in(own, position), (blocks,), jnp.float32, smallest / len(shards), top_value / len(shards)))
        loudness = loudness * jnp.repeat(steps, dims[position] // blocks).reshape([-1 if axis == position else 1 for axis in range(len(dims))])
    return loudness


def centred(stream_key, dims, scale, limit, cuts=(), kind=jnp.bfloat16):
    result = scale * jax.random.normal(stream_key, dims, jnp.float32)
    if cuts:
        result = result * block_scale(stream_key, dims, cuts, -0.22, 0.18)
    return jnp.clip(result, -limit, limit).astype(kind)


def setup_inputs(seed: int = 0) -> dict:
    arg_keys = jax.random.split(jax.random.key(seed), 16)
    tokens = centred(arg_keys[0], (SEQS, LEN, D), 1.0, 6.0, ((0, 4), (1, 4), (2, 2)))
    norm_gain = jnp.clip(1.0 + 0.18 * jax.random.normal(arg_keys[1], (D,), jnp.float32), 0.1, 1.9)
    query_weight = centred(arg_keys[2], (D, HEADS * DK), D ** -0.5, 0.125, ((0, 16), (1, 2)))
    key_weight = centred(arg_keys[3], (D, HEADS * DK), D ** -0.5, 0.125, ((0, 16), (1, 2)))
    value_weight = centred(arg_keys[4], (D, HEADS * DV), D ** -0.5, 0.125, ((0, 16), (1, 2)))
    outgate_weight = centred(arg_keys[5], (D, HEADS * DV), D ** -0.5, 0.125, ((0, 16), (1, 2)))
    gate_weight = draw_gate_weight(jax.random.fold_in(arg_keys[15], 71), 0)
    forget_bias = draw_forget_bias(jax.random.fold_in(arg_keys[15], 71), 0)
    forget_shift = draw_forget_shift(jax.random.fold_in(arg_keys[15], 71), 0)
    head_norm_gain = jnp.clip(1.0 + 0.18 * jax.random.normal(arg_keys[9], (HEADS * DV,), jnp.float32), 0.1, 1.9)
    exit_weight = centred(arg_keys[10], (D, CONV), D ** -0.5, 0.125, ((0, 16), (1, 2)))
    entry_weight = centred(arg_keys[11], (D, CONV), D ** -0.5, 0.125, ((0, 16), (1, 2)))
    signal_weight = centred(arg_keys[12], (D, CONV), D ** -0.5, 0.125, ((0, 16), (1, 2)))
    conv_kernel = centred(arg_keys[13], (KERNEL, CONV), KERNEL ** -0.5, 3.5, ((1, 2),), jnp.float32)
    merge_weight = centred(arg_keys[14], (HEADS * DV + CONV, D), (HEADS * DV + CONV) ** -0.5, 0.09375, ((0, 16), (1, 2)))
    return {"tokens": tokens, "norm_gain": norm_gain, "query_weight": query_weight, "key_weight": key_weight, "value_weight": value_weight, "outgate_weight": outgate_weight, "gate_weight": gate_weight, "forget_bias": forget_bias, "forget_shift": forget_shift, "head_norm_gain": head_norm_gain, "exit_weight": exit_weight, "entry_weight": entry_weight, "signal_weight": signal_weight, "conv_kernel": conv_kernel, "merge_weight": merge_weight}


EPSILON = 1e-06
HIGHEST = lax.Precision.HIGHEST

def reference(tokens, norm_gain, query_weight, key_weight, value_weight, outgate_weight, gate_weight, forget_bias, forget_shift, head_norm_gain, exit_weight, entry_weight, signal_weight, conv_kernel, merge_weight):
    count = SEQS * LEN
    blocks = LEN // BLOCK
    flat = tokens.astype(jnp.float32)
    normed = (flat * lax.rsqrt(lax.optimization_barrier(jnp.mean(flat * flat, axis=-1, keepdims=True)) + EPSILON) * norm_gain).astype(jnp.bfloat16)
    rows = normed.reshape(count, D)

    def project(weight):
        return jnp.dot(rows, weight, preferred_element_type=jnp.float32)
    queries = project(query_weight).astype(jnp.bfloat16)
    keys = project(key_weight).astype(jnp.bfloat16)
    values = project(value_weight).astype(jnp.bfloat16)
    outgates = project(outgate_weight).astype(jnp.bfloat16)
    exit_rows = project(exit_weight).astype(jnp.bfloat16)
    entry_rows = project(entry_weight).astype(jnp.bfloat16)
    signal_rows = project(signal_weight).astype(jnp.bfloat16)
    gates = project(gate_weight.reshape(D, 2 * HEADS))

    def split_heads(array, width):
        return array.reshape(SEQS, blocks, BLOCK, HEADS, width).transpose(0, 3, 1, 2, 4).astype(jnp.float32)

    def lanes(array):
        return array.reshape(SEQS, blocks, BLOCK, HEADS).transpose(0, 3, 1, 2)
    inputs = lanes(gates[:, :HEADS])
    logs = lanes(jax.nn.log_sigmoid(gates[:, HEADS:] + forget_bias)) + forget_shift.reshape(SEQS, HEADS, blocks, BLOCK)
    query_float = split_heads(queries, DK)
    key_float = split_heads(keys, DK)
    value_float = split_heads(values, DV)
    scale = DK ** (-0.5)
    cumulative = jnp.cumsum(logs, axis=-1)
    last = cumulative[..., -1]
    weight_logs = last[..., None] - cumulative + inputs
    peak = lax.optimization_barrier(jnp.max(weight_logs, axis=-1))
    coefficient_array = jnp.exp(weight_logs - peak[..., None])
    scaled = key_float * scale
    states = jnp.einsum('bhcs,bhcsk,bhcsv->bhckv', coefficient_array, scaled, value_float, precision=HIGHEST)

    def step(carry, item):
        state, bounded_maximum = carry
        block_last, block_peak, block_state = item
        ceiling = jnp.maximum(block_last + bounded_maximum, block_peak)
        kept = jnp.exp(block_last + bounded_maximum - ceiling)
        added = jnp.exp(block_peak - ceiling)
        new_state = kept[..., None, None] * state + added[..., None, None] * block_state
        return ((new_state, ceiling), (state, bounded_maximum))
    start = (jnp.zeros((SEQS, HEADS, DK, DV), jnp.float32), jnp.zeros((SEQS, HEADS), jnp.float32))
    items = (jnp.moveaxis(last, 2, 0), jnp.moveaxis(peak, 2, 0), jnp.moveaxis(states, 2, 0))
    unused, before = lax.scan(step, start, items)
    state_prev = jnp.moveaxis(before[0], 0, 2)
    stable_prev = jnp.moveaxis(before[1], 0, 2)
    score_matrix = jnp.einsum('bhcjk,bhcsk->bhcjs', query_float, key_float) * scale
    causal = jnp.tril(jnp.ones((BLOCK, BLOCK), dtype=bool))
    decay = jnp.where(causal, cumulative[..., :, None] - cumulative[..., None, :] + inputs[..., None, :], -jnp.inf)
    inter = cumulative + stable_prev[..., None]
    ceiling = jnp.maximum(inter, lax.optimization_barrier(jnp.max(decay, axis=-1)))
    weighted = score_matrix * jnp.exp(decay - ceiling[..., None])
    rounded = lax.optimization_barrier(weighted.astype(jnp.bfloat16)).astype(jnp.float32)
    carried = jnp.exp(inter - ceiling)
    numerator = jnp.einsum('bhcjs,bhcsv->bhcjv', rounded, value_float)
    numerator = numerator + carried[..., None] * jnp.einsum('bhcjk,bhckv->bhcjv', query_float, state_prev, precision=HIGHEST)
    hidden = numerator * lax.rsqrt(lax.optimization_barrier(jnp.mean(numerator * numerator, axis=-1, keepdims=True)) + EPSILON)
    hidden = hidden.transpose(0, 2, 3, 1, 4).reshape(count, HEADS * DV) * head_norm_gain
    memory_out = (hidden * jax.nn.sigmoid(outgates.astype(jnp.float32))).astype(jnp.bfloat16)
    mixed_in = (entry_rows.astype(jnp.float32) * signal_rows.astype(jnp.float32)).astype(jnp.bfloat16)
    padded = jnp.pad(mixed_in.reshape(SEQS, LEN, CONV).astype(jnp.float32), ((0, 0), (KERNEL - 1, 0), (0, 0)))
    response = jnp.zeros((SEQS, LEN, CONV), jnp.float32)
    for tap in range(KERNEL):
        response = response + conv_kernel[tap] * padded[:, tap:tap + LEN]
    conv_out = (exit_rows.astype(jnp.float32) * response.reshape(count, CONV)).astype(jnp.bfloat16)
    concatenated_result = jnp.concatenate([memory_out, conv_out], axis=1)
    mixed = jnp.dot(concatenated_result, merge_weight, preferred_element_type=jnp.float32).astype(jnp.bfloat16)
    return mixed.reshape(SEQS, LEN, D)
```

```python
import jax
import jax.numpy as jnp
from jax import lax
from jax.sharding import PartitionSpec as P

DK = 64
DV = 128
BLOCK = 128
KERNEL = 3


EPSILON = 1e-06
EMPTY_LOG = -1e30
HIGHEST = lax.Precision.HIGHEST


def prefix(part, axis, combine, identity):
    place = lax.axis_index(axis)
    gathered = jax.tree.map(lambda a: lax.all_gather(a, axis), part)
    state = jax.tree.map(lambda a, e: jnp.zeros_like(a) + jnp.asarray(e, a.dtype), part, identity)

    def one(step, state):
        return combine(
            state, jax.tree.map(lambda a: lax.dynamic_index_in_dim(a, step, 0, False), gathered)
        )

    return lax.fori_loop(0, place, one, state)


def passed_along(value, axis, steps):
    count = lax.axis_size(axis)
    initial, last = (max(0, -steps), min(count, count - steps))
    return lax.ppermute(value, axis, [(source, source + steps) for source in range(initial, last)])


def combine(earlier, later):
    ceiling = jnp.maximum(later[2] + earlier[1], later[1])
    kept = jnp.exp(later[2] + earlier[1] - ceiling)
    added = jnp.exp(later[1] - ceiling)
    state = kept[..., None, None] * earlier[0] + added[..., None, None] * later[0]
    return (state, ceiling, earlier[2] + later[2])


def identity_state(heads):
    return (
        jnp.zeros((heads, DK, DV), jnp.float32),
        jnp.full((heads,), EMPTY_LOG, jnp.float32),
        jnp.zeros((heads,), jnp.float32),
    )


def add_product(left, piece):
    return jnp.dot(left, piece, preferred_element_type=jnp.float32)


def split_columns(total, stack):
    outputs = []
    offset = 0
    for weight in stack:
        outputs.append(total[:, offset : offset + weight.shape[1]])
        offset = offset + weight.shape[1]
    return outputs


def incoming_state(running):
    heads = running[1].shape[0]
    before = prefix((running[0], running[1], running[2]), "sp", combine, identity_state(heads))
    ceiling = jnp.maximum(before[1], before[2])
    shrink = jnp.exp(before[1] - ceiling)
    return (before[0] * shrink[:, None, None], ceiling, before[2])


def memory_states(keys, values, gates, forget_bias, forget_shift):
    count = gates.shape[0]
    heads = forget_bias.shape[0]
    blocks = count // BLOCK
    inputs = gates[:, :heads].reshape(blocks, BLOCK, heads)
    logs = jax.nn.log_sigmoid(gates[:, heads:] + forget_bias) + forget_shift[0].T
    cumulative = jnp.cumsum(logs.reshape(blocks, BLOCK, heads), axis=1)
    last = cumulative[:, -1]
    weight_logs = last[:, None, :] - cumulative + inputs
    peak = jnp.max(weight_logs, axis=1)
    coefficient_array = jnp.exp(weight_logs - peak[:, None, :])
    scaled = keys.reshape(blocks, BLOCK, heads, DK).astype(jnp.float32) * DK ** (-0.5)
    value_float = values.reshape(blocks, BLOCK, heads, DV).astype(jnp.float32)
    states = jnp.einsum(
        "csh,cshk,cshv->chkv", coefficient_array, scaled, value_float, precision=HIGHEST
    )
    running = identity_state(heads)
    prefixes = []
    for index in range(blocks):
        prefixes.append(running)
        running = combine(running, (states[index], peak[index], last[index]))
    leading_part = tuple((jnp.stack([item[member] for item in prefixes]) for member in range(3)))
    gate_apertures = combine(incoming_state(running), leading_part)
    return (gate_apertures, cumulative, inputs)


def memory_output(
    queries, keys, values, outgates, inputs, cumulative, gate_apertures, head_norm_gain
):
    blocks = cumulative.shape[0]
    heads = cumulative.shape[2]
    count = queries.shape[0]
    query_blocks = queries.reshape(blocks, BLOCK, heads, DK)
    key_blocks = keys.reshape(blocks, BLOCK, heads, DK)
    value_blocks = values.reshape(blocks, BLOCK, heads, DV)
    score_matrix = jnp.einsum(
        "cjhk,cshk->chjs", query_blocks, key_blocks, preferred_element_type=jnp.float32
    ) * DK ** (-0.5)
    cum_lanes = cumulative.transpose(0, 2, 1)
    input_lanes = inputs.transpose(0, 2, 1)
    causal = jnp.tril(jnp.ones((BLOCK, BLOCK), dtype=bool))
    decay = jnp.where(
        causal,
        cum_lanes[..., :, None] - cum_lanes[..., None, :] + input_lanes[..., None, :],
        -jnp.inf,
    )
    inter = cum_lanes + gate_apertures[1][..., None]
    ceiling = jnp.maximum(inter, jnp.max(decay, axis=-1))
    weighted = score_matrix * jnp.exp(decay - ceiling[..., None])
    numerator = jnp.einsum(
        "chjs,cshv->chjv",
        weighted.astype(jnp.bfloat16),
        value_blocks,
        preferred_element_type=jnp.float32,
    )
    query_float = query_blocks.astype(jnp.float32)
    carried = jnp.exp(inter - ceiling)
    numerator = numerator + carried[..., None] * jnp.einsum(
        "cjhk,chkv->chjv", query_float, gate_apertures[0], precision=HIGHEST
    )
    result = numerator * lax.rsqrt(
        jnp.mean(numerator * numerator, axis=-1, keepdims=True) + EPSILON
    )
    result = result.transpose(0, 2, 1, 3).reshape(count, heads * DV) * head_norm_gain
    return (result * jax.nn.sigmoid(outgates.astype(jnp.float32))).astype(jnp.bfloat16)


def by_position(
    tokens,
    norm_gain,
    query_weight,
    key_weight,
    value_weight,
    outgate_weight,
    gate_weight,
    forget_bias,
    forget_shift,
    head_norm_gain,
    exit_weight,
    entry_weight,
    signal_weight,
    conv_kernel,
    merge_weight,
):
    whole = lax.all_gather(tokens, "tp", axis=2, tiled=True)[0]
    count = whole.shape[0]
    flat = whole.astype(jnp.float32)
    normed = (
        flat * lax.rsqrt(jnp.mean(flat * flat, axis=-1, keepdims=True) + EPSILON) * norm_gain
    ).astype(jnp.bfloat16)
    gate_rows = gate_weight.reshape(gate_weight.shape[0], -1)
    state_stack = [key_weight, value_weight, gate_rows]
    other_stack = [query_weight, outgate_weight, exit_weight, entry_weight, signal_weight]
    stacked = jnp.concatenate(state_stack + other_stack, axis=1)
    total = add_product(normed, lax.all_gather(stacked, ("sp", "fs"), axis=0, tiled=True))
    columns = split_columns(total, state_stack + other_stack)
    keys = columns[0].astype(jnp.bfloat16)
    values = columns[1].astype(jnp.bfloat16)
    gate_apertures, cumulative, inputs = memory_states(
        keys, values, columns[2], forget_bias, forget_shift
    )
    others = columns[3:]
    queries = others[0].astype(jnp.bfloat16)
    outgates = others[1].astype(jnp.bfloat16)
    exit_rows = others[2].astype(jnp.bfloat16)
    entry_rows = others[3].astype(jnp.bfloat16)
    signal_rows = others[4].astype(jnp.bfloat16)
    mixed_in = (entry_rows.astype(jnp.float32) * signal_rows.astype(jnp.float32)).astype(
        jnp.bfloat16
    )
    rim = passed_along(mixed_in[count - (KERNEL - 1) :], "sp", 1)
    padded = jnp.concatenate([rim, mixed_in], axis=0).astype(jnp.float32)
    response = conv_kernel[0] * padded[0:count]
    for tap in range(1, KERNEL):
        response = response + conv_kernel[tap] * padded[tap : tap + count]
    conv_out = (exit_rows.astype(jnp.float32) * response).astype(jnp.bfloat16)
    memory_out = memory_output(
        queries, keys, values, outgates, inputs, cumulative, gate_apertures, head_norm_gain
    )
    memory_all, conv_all = (
        lax.all_gather(memory_out, "tp", axis=1, tiled=True),
        lax.all_gather(conv_out, "tp", axis=1, tiled=True),
    )
    concatenated_result = jnp.concatenate([memory_all, conv_all], axis=1)
    mixed = add_product(
        concatenated_result, lax.all_gather(merge_weight, ("sp", "fs"), axis=0, tiled=True)
    )
    return mixed.astype(jnp.bfloat16)[None]


def own_part(value, axis, place, count):
    size = value.shape[axis] // count
    return lax.dynamic_slice_in_dim(value, place * size, size, axis)


def dealt(value, axis):
    return lax.all_to_all(value, axis, 0, 0, tiled=True)


def along_line(value, axis):
    count = lax.axis_size(axis)
    place = lax.axis_index(axis)
    up = [value]
    down = [value]
    for step in range(1, count):
        up.append(lax.ppermute(up[-1], axis, [(i, i + 1) for i in range(step - 1, count - 1)]))
        down.append(lax.ppermute(down[-1], axis, [(i, i - 1) for i in range(1, count - step + 1)]))
    return [value] + [
        jnp.where(place >= step, up[step], down[count - step]) for step in range(1, count)
    ]


def summed_on_line(part, axis):
    count = lax.axis_size(axis)
    place = lax.axis_index(axis)
    up = down = None
    for step in range(1, count):
        above = part(jnp.minimum(place + count - step, count - 1))
        below = part(jnp.maximum(place - count + step, 0))
        if step > 1:
            above = above + up.astype(jnp.float32)
            below = below + down.astype(jnp.float32)
        up = lax.ppermute(
            above.astype(jnp.bfloat16), axis, [(i, i + 1) for i in range(min(step, count - 1))]
        )
        down = lax.ppermute(
            below.astype(jnp.bfloat16),
            axis,
            [(i, i - 1) for i in range(count - 1, count - 1 - step, -1)],
        )
    return part(place) + up.astype(jnp.float32) + down.astype(jnp.float32)


def swapped(value):
    return lax.ppermute(value, "tp", [(0, 1), (1, 0)])


def carried_states(states, peak, last):
    blocks = last.shape[0]
    index = jnp.arange(blocks)
    after = (index[None, None, :] > index[None, :, None]) & (
        index[None, None, :] < index[:, None, None]
    )
    between = jnp.sum(jnp.where(after[..., None], last[None, None], 0.0), axis=2)
    before = index[None, :] < index[:, None]
    start = jnp.sum(jnp.where(before[..., None], last[None], 0.0), axis=1)
    logs = jnp.where(before[..., None], between + peak[None], EMPTY_LOG)
    ceiling = jnp.maximum(start, jnp.max(logs, axis=1))
    factors = jnp.where(before[..., None], jnp.exp(logs - ceiling[:, None]), 0.0)
    state = jnp.einsum("cbh,bhkv->chkv", factors, states, precision=HIGHEST)
    return (state, ceiling)


def sequence_states(keys, values, gates, forget_bias, forget_shift):
    count = gates.shape[0]
    heads = forget_bias.shape[0]
    blocks = count // BLOCK
    inputs = gates[:, :heads].reshape(blocks, BLOCK, heads)
    logs = jax.nn.log_sigmoid(gates[:, heads:] + forget_bias) + forget_shift.T
    cumulative = jnp.cumsum(logs.reshape(blocks, BLOCK, heads), axis=1)
    last = cumulative[:, -1]
    weight_logs = last[:, None, :] - cumulative + inputs
    peak = jnp.max(weight_logs, axis=1)
    coefficient_array = jnp.exp(weight_logs - peak[:, None, :])
    scaled = keys.reshape(blocks, BLOCK, heads, DK).astype(jnp.float32) * DK ** (-0.5)
    value_float = values.reshape(blocks, BLOCK, heads, DV).astype(jnp.float32)
    states = jnp.einsum(
        "csh,cshk,cshv->chkv", coefficient_array, scaled, value_float, precision=HIGHEST
    )
    return (carried_states(states, peak, last), cumulative, inputs)


def by_sequence(
    tokens,
    norm_gain,
    query_weight,
    key_weight,
    value_weight,
    outgate_weight,
    gate_weight,
    forget_bias,
    forget_shift,
    head_norm_gain,
    exit_weight,
    entry_weight,
    signal_weight,
    conv_kernel,
    merge_weight,
):
    count = lax.axis_size("sp")
    place = lax.axis_index("sp")
    side = lax.axis_index("tp")
    rows = tokens.shape[1]
    half = tokens.shape[2]

    def pieces(weight):
        weight = weight.reshape(weight.shape[0], count, -1)
        return weight.transpose(1, 0, 2)

    gate_pieces = gate_weight.reshape(gate_weight.shape[0], 2, count, -1).transpose(2, 0, 1, 3)
    gate_pieces = gate_pieces.reshape(count, gate_weight.shape[0], -1)
    first_stack = [query_weight, key_weight, value_weight]
    spare = -gate_pieces.shape[2] % 128
    gate_pieces = jnp.pad(gate_pieces, ((0, 0), (0, 0), (0, spare)))
    first = jnp.concatenate([pieces(w) for w in first_stack] + [gate_pieces], axis=2)
    second_stack = [outgate_weight, exit_weight, entry_weight, signal_weight]
    second = jnp.concatenate([pieces(w) for w in second_stack], axis=2)
    first = dealt(first, "sp")
    second = dealt(second, "sp")

    mine = tokens[0]
    normed = jnp.zeros((count, rows, 2 * half), jnp.bfloat16)
    for step, chunk in enumerate(along_line(mine, "sp")):
        other = swapped(chunk)
        flat = jnp.concatenate(
            [jnp.where(side == 0, chunk, other), jnp.where(side == 0, other, chunk)], axis=1
        ).astype(jnp.float32)
        flat = flat * lax.rsqrt(jnp.mean(flat * flat, axis=-1, keepdims=True) + EPSILON)
        normed = lax.dynamic_update_slice_in_dim(
            normed, (flat * norm_gain).astype(jnp.bfloat16)[None], (place - step) % count, 0
        )
    normed = normed.reshape(count * rows, 2 * half)

    shifts = forget_shift[0].reshape(count, -1, rows)
    shifts = dealt(shifts, "sp").transpose(1, 0, 2).reshape(-1, count * rows)

    first = lax.all_gather(first, "fs", axis=1, tiled=True).reshape(2 * half, -1)
    second = lax.all_gather(second, "fs", axis=1, tiled=True).reshape(2 * half, -1)
    merge = lax.ppermute(
        merge_weight,
        ("sp", "fs"),
        [(i * count + j, j * count + i) for i in range(count) for j in range(count)],
    )
    merge = lax.all_gather(merge, "fs", axis=0)

    total = add_product(normed, first)
    width = query_weight.shape[1] // count
    queries = total[:, :width].astype(jnp.bfloat16)
    keys = total[:, width : 2 * width].astype(jnp.bfloat16)
    deep = value_weight.shape[1] // count
    values = total[:, 2 * width : 2 * width + deep].astype(jnp.bfloat16)
    gates = total[:, 2 * width + deep : total.shape[1] - spare]
    gate_apertures, cumulative, inputs = sequence_states(
        keys, values, gates, own_part(forget_bias, 0, place, count), shifts
    )

    others = add_product(normed, second).astype(jnp.bfloat16)
    channels = exit_weight.shape[1] // count
    outgates = others[:, :deep]
    exit_rows = others[:, deep : deep + channels]
    entry_rows = others[:, deep + channels : deep + 2 * channels]
    signal_rows = others[:, deep + 2 * channels :]
    mixed_in = (entry_rows.astype(jnp.float32) * signal_rows.astype(jnp.float32)).astype(
        jnp.bfloat16
    )
    length = mixed_in.shape[0]
    padded = jnp.pad(mixed_in, ((KERNEL - 1, 0), (0, 0))).astype(jnp.float32)
    taps = own_part(conv_kernel, 1, place, count)
    response = taps[0] * padded[0:length]
    for tap in range(1, KERNEL):
        response = response + taps[tap] * padded[tap : tap + length]
    conv_out = (exit_rows.astype(jnp.float32) * response).astype(jnp.bfloat16)
    conv_other = swapped(conv_out)
    memory_out = memory_output(
        queries,
        keys,
        values,
        outgates,
        inputs,
        cumulative,
        gate_apertures,
        own_part(head_norm_gain, 0, place, count),
    )
    memory_other = swapped(memory_out)
    features = jnp.concatenate([memory_out, memory_other, conv_out, conv_other], axis=1)
    features = features.reshape(count, rows, -1)
    flipped = jnp.stack([merge[1], merge[0], merge[3], merge[2]])
    turned = jnp.where(side == 0, merge, flipped)
    turned = turned.reshape(-1, merge.shape[2])

    def part(member):
        return add_product(lax.dynamic_index_in_dim(features, member, 0, False), turned)

    mixed = summed_on_line(part, "sp")
    return mixed.astype(jnp.bfloat16)[None]


def local(*arguments):
    count = lax.axis_size("sp")
    merge_rows = arguments[14].shape[0]
    fits = (
        lax.axis_size("tp") == 2
        and lax.axis_size("fs") == count
        and count == 4
        and arguments[7].shape[0] % count == 0
        and merge_rows == arguments[4].shape[1] // count
        and merge_rows == arguments[10].shape[1] // count
    )
    return by_sequence(*arguments) if fits else by_position(*arguments)


def solution(mesh):
    placed = (
        P("fs", "sp", "tp"),
        P(),
        P(("sp", "fs"), "tp"),
        P(("sp", "fs"), "tp"),
        P(("sp", "fs"), "tp"),
        P(("sp", "fs"), "tp"),
        P(("sp", "fs"), None, "tp"),
        P("tp"),
        P("fs", "tp", "sp"),
        P("tp"),
        P(("sp", "fs"), "tp"),
        P(("sp", "fs"), "tp"),
        P(("sp", "fs"), "tp"),
        P(None, "tp"),
        P(("sp", "fs"), "tp"),
    )
    return jax.shard_map(
        local, mesh=mesh, in_specs=placed, out_specs=P("fs", "sp", "tp"), check_vma=False
    )
```

```python
import jax
import jax.numpy as jnp
from jax import lax
from jax.sharding import PartitionSpec as P

DK = 64
DV = 128
BLOCK = 128
KERNEL = 3


EPSILON = 1e-06
EMPTY_LOG = -1e30
HIGHEST = lax.Precision.HIGHEST


def prefix(part, axis, combine, identity):
    place = lax.axis_index(axis)
    gathered = jax.tree.map(lambda a: lax.all_gather(a, axis), part)
    state = jax.tree.map(lambda a, e: jnp.zeros_like(a) + jnp.asarray(e, a.dtype), part, identity)

    def one(step, state):
        return combine(
            state, jax.tree.map(lambda a: lax.dynamic_index_in_dim(a, step, 0, False), gathered)
        )

    return lax.fori_loop(0, place, one, state)


def passed_along(value, axis, steps):
    count = lax.axis_size(axis)
    initial, last = (max(0, -steps), min(count, count - steps))
    return lax.ppermute(value, axis, [(source, source + steps) for source in range(initial, last)])


def combine(earlier, later):
    ceiling = jnp.maximum(later[2] + earlier[1], later[1])
    kept = jnp.exp(later[2] + earlier[1] - ceiling)
    added = jnp.exp(later[1] - ceiling)
    state = kept[..., None, None] * earlier[0] + added[..., None, None] * later[0]
    return (state, ceiling, earlier[2] + later[2])


def identity_state(heads):
    return (
        jnp.zeros((heads, DK, DV), jnp.float32),
        jnp.full((heads,), EMPTY_LOG, jnp.float32),
        jnp.zeros((heads,), jnp.float32),
    )


def add_product(left, piece):
    return jnp.dot(left, piece, preferred_element_type=jnp.float32)


def split_columns(total, stack):
    outputs = []
    offset = 0
    for weight in stack:
        outputs.append(total[:, offset : offset + weight.shape[1]])
        offset = offset + weight.shape[1]
    return outputs


def incoming_state(running):
    heads = running[1].shape[0]
    before = prefix((running[0], running[1], running[2]), "sp", combine, identity_state(heads))
    ceiling = jnp.maximum(before[1], before[2])
    shrink = jnp.exp(before[1] - ceiling)
    return (before[0] * shrink[:, None, None], ceiling, before[2])


def memory_states(keys, values, gates, forget_bias, forget_shift):
    count = gates.shape[0]
    heads = forget_bias.shape[0]
    blocks = count // BLOCK
    inputs = gates[:, :heads].reshape(blocks, BLOCK, heads)
    logs = jax.nn.log_sigmoid(gates[:, heads:] + forget_bias) + forget_shift[0].T
    cumulative = jnp.cumsum(logs.reshape(blocks, BLOCK, heads), axis=1)
    last = cumulative[:, -1]
    weight_logs = last[:, None, :] - cumulative + inputs
    peak = jnp.max(weight_logs, axis=1)
    coefficient_array = jnp.exp(weight_logs - peak[:, None, :])
    scaled = keys.reshape(blocks, BLOCK, heads, DK).astype(jnp.float32) * DK ** (-0.5)
    value_float = values.reshape(blocks, BLOCK, heads, DV).astype(jnp.float32)
    states = jnp.einsum(
        "csh,cshk,cshv->chkv", coefficient_array, scaled, value_float, precision=HIGHEST
    )
    running = identity_state(heads)
    prefixes = []
    for index in range(blocks):
        prefixes.append(running)
        running = combine(running, (states[index], peak[index], last[index]))
    leading_part = tuple((jnp.stack([item[member] for item in prefixes]) for member in range(3)))
    gate_apertures = combine(incoming_state(running), leading_part)
    return (gate_apertures, cumulative, inputs)


def memory_output(
    queries, keys, values, outgates, inputs, cumulative, gate_apertures, head_norm_gain
):
    blocks = cumulative.shape[0]
    heads = cumulative.shape[2]
    count = queries.shape[0]
    query_blocks = queries.reshape(blocks, BLOCK, heads, DK)
    key_blocks = keys.reshape(blocks, BLOCK, heads, DK)
    value_blocks = values.reshape(blocks, BLOCK, heads, DV)
    score_matrix = jnp.einsum(
        "cjhk,cshk->chjs", query_blocks, key_blocks, preferred_element_type=jnp.float32
    ) * DK ** (-0.5)
    cum_lanes = cumulative.transpose(0, 2, 1)
    input_lanes = inputs.transpose(0, 2, 1)
    causal = jnp.tril(jnp.ones((BLOCK, BLOCK), dtype=bool))
    decay = jnp.where(
        causal,
        cum_lanes[..., :, None] - cum_lanes[..., None, :] + input_lanes[..., None, :],
        -jnp.inf,
    )
    inter = cum_lanes + gate_apertures[1][..., None]
    ceiling = jnp.maximum(inter, jnp.max(decay, axis=-1))
    weighted = score_matrix * jnp.exp(decay - ceiling[..., None])
    numerator = jnp.einsum(
        "chjs,cshv->chjv",
        weighted.astype(jnp.bfloat16),
        value_blocks,
        preferred_element_type=jnp.float32,
    )
    query_float = query_blocks.astype(jnp.float32)
    carried = jnp.exp(inter - ceiling)
    numerator = numerator + carried[..., None] * jnp.einsum(
        "cjhk,chkv->chjv", query_float, gate_apertures[0], precision=HIGHEST
    )
    result = numerator * lax.rsqrt(
        jnp.mean(numerator * numerator, axis=-1, keepdims=True) + EPSILON
    )
    result = result.transpose(0, 2, 1, 3).reshape(count, heads * DV) * head_norm_gain
    return (result * jax.nn.sigmoid(outgates.astype(jnp.float32))).astype(jnp.bfloat16)


def by_position(
    tokens,
    norm_gain,
    query_weight,
    key_weight,
    value_weight,
    outgate_weight,
    gate_weight,
    forget_bias,
    forget_shift,
    head_norm_gain,
    exit_weight,
    entry_weight,
    signal_weight,
    conv_kernel,
    merge_weight,
):
    whole = lax.all_gather(tokens, "tp", axis=2, tiled=True)[0]
    count = whole.shape[0]
    flat = whole.astype(jnp.float32)
    normed = (
        flat * lax.rsqrt(jnp.mean(flat * flat, axis=-1, keepdims=True) + EPSILON) * norm_gain
    ).astype(jnp.bfloat16)
    gate_rows = gate_weight.reshape(gate_weight.shape[0], -1)
    state_stack = [key_weight, value_weight, gate_rows]
    other_stack = [query_weight, outgate_weight, exit_weight, entry_weight, signal_weight]
    stacked = jnp.concatenate(state_stack + other_stack, axis=1)
    total = add_product(normed, lax.all_gather(stacked, ("sp", "fs"), axis=0, tiled=True))
    columns = split_columns(total, state_stack + other_stack)
    keys = columns[0].astype(jnp.bfloat16)
    values = columns[1].astype(jnp.bfloat16)
    gate_apertures, cumulative, inputs = memory_states(
        keys, values, columns[2], forget_bias, forget_shift
    )
    others = columns[3:]
    queries = others[0].astype(jnp.bfloat16)
    outgates = others[1].astype(jnp.bfloat16)
    exit_rows = others[2].astype(jnp.bfloat16)
    entry_rows = others[3].astype(jnp.bfloat16)
    signal_rows = others[4].astype(jnp.bfloat16)
    mixed_in = (entry_rows.astype(jnp.float32) * signal_rows.astype(jnp.float32)).astype(
        jnp.bfloat16
    )
    rim = passed_along(mixed_in[count - (KERNEL - 1) :], "sp", 1)
    padded = jnp.concatenate([rim, mixed_in], axis=0).astype(jnp.float32)
    response = conv_kernel[0] * padded[0:count]
    for tap in range(1, KERNEL):
        response = response + conv_kernel[tap] * padded[tap : tap + count]
    conv_out = (exit_rows.astype(jnp.float32) * response).astype(jnp.bfloat16)
    memory_out = memory_output(
        queries, keys, values, outgates, inputs, cumulative, gate_apertures, head_norm_gain
    )
    memory_all, conv_all = (
        lax.all_gather(memory_out, "tp", axis=1, tiled=True),
        lax.all_gather(conv_out, "tp", axis=1, tiled=True),
    )
    concatenated_result = jnp.concatenate([memory_all, conv_all], axis=1)
    mixed = add_product(
        concatenated_result, lax.all_gather(merge_weight, ("sp", "fs"), axis=0, tiled=True)
    )
    return mixed.astype(jnp.bfloat16)[None]


def own_part(value, axis, place, count):
    size = value.shape[axis] // count
    return lax.dynamic_slice_in_dim(value, place * size, size, axis)


def dealt(value, axis):
    return lax.all_to_all(value, axis, 0, 0, tiled=True)


def traded(value, axis, step):
    count = lax.axis_size(axis)
    return lax.ppermute(value, axis, [(i, i ^ step) for i in range(count)])


def swapped(value):
    return lax.ppermute(value, "tp", [(0, 1), (1, 0)])


def earlier_members(running):
    place = lax.axis_index("sp")
    rows = running[0].shape[1] // 2
    gathered = jnp.concatenate(
        [
            lax.all_gather(running[0][:, :rows], "sp"),
            lax.all_gather(running[0][:, rows:], "sp"),
        ],
        axis=2,
    )
    logs = lax.all_gather(jnp.stack(running[1:]), "sp")
    state = identity_state(running[1].shape[0])
    for index in range(lax.axis_size("sp")):
        after = combine(state, (gathered[index], logs[index, 0], logs[index, 1]))
        state = tuple(jnp.where(index < place, a, b) for a, b in zip(after, state))
    ceiling = jnp.maximum(state[1], state[2])
    return (state[0] * jnp.exp(state[1] - ceiling)[:, None, None], ceiling, state[2])


def plane_states(keys, values, gates, forget_bias, forget_shift, sequences):
    count = gates.shape[0]
    heads = forget_bias.shape[0]
    blocks = count // BLOCK
    inputs = gates[:, :heads].reshape(blocks, BLOCK, heads)
    logs = jax.nn.log_sigmoid(gates[:, heads:] + forget_bias) + forget_shift
    cumulative = jnp.cumsum(logs.reshape(blocks, BLOCK, heads), axis=1)
    last = cumulative[:, -1]
    weight_logs = last[:, None, :] - cumulative + inputs
    peak = jnp.max(weight_logs, axis=1)
    coefficient_array = jnp.exp(weight_logs - peak[:, None, :])
    scaled = keys.reshape(blocks, BLOCK, heads, DK).astype(jnp.float32) * DK ** (-0.5)
    value_float = values.reshape(blocks, BLOCK, heads, DV).astype(jnp.float32)
    states = jnp.einsum(
        "csh,cshk,cshv->chkv", coefficient_array, scaled, value_float, precision=HIGHEST
    )

    def by_block(array):
        array = array.reshape(sequences, -1, *array.shape[1:]).swapaxes(0, 1)
        return array.reshape(array.shape[0], -1, *array.shape[3:])

    def flat_blocks(array):
        array = array.reshape(array.shape[0], sequences, heads, *array.shape[2:])
        return array.swapaxes(0, 1).reshape(blocks, heads, *array.shape[3:])

    states, peak, last = by_block(states), by_block(peak), by_block(last)
    running = identity_state(sequences * heads)
    prefixes = []
    for index in range(states.shape[0]):
        prefixes.append(running)
        running = combine(running, (states[index], peak[index], last[index]))
    leading_part = tuple((jnp.stack([item[member] for item in prefixes]) for member in range(3)))
    before = combine(earlier_members(running), leading_part)
    return (tuple(flat_blocks(item) for item in before[:2]), cumulative, inputs)


def by_plane(
    tokens,
    norm_gain,
    query_weight,
    key_weight,
    value_weight,
    outgate_weight,
    gate_weight,
    forget_bias,
    forget_shift,
    head_norm_gain,
    exit_weight,
    entry_weight,
    signal_weight,
    conv_kernel,
    merge_weight,
):
    count = lax.axis_size("fs")
    place = lax.axis_index("fs")
    side = lax.axis_index("tp")
    rows = tokens.shape[1]
    half = tokens.shape[2]

    def pieces(weight):
        weight = weight.reshape(weight.shape[0], count, -1)
        return weight.transpose(1, 0, 2)

    gate_pieces = gate_weight.reshape(gate_weight.shape[0], 2, count, -1).transpose(2, 0, 1, 3)
    gate_pieces = gate_pieces.reshape(count, gate_weight.shape[0], -1)
    first_stack = [query_weight, key_weight, value_weight]
    spare = -gate_pieces.shape[2] % 128
    gate_pieces = jnp.pad(gate_pieces, ((0, 0), (0, 0), (0, spare)))
    first = jnp.concatenate([pieces(w) for w in first_stack] + [gate_pieces], axis=2)
    second_stack = [outgate_weight, exit_weight, entry_weight, signal_weight]
    second = jnp.concatenate([pieces(w) for w in second_stack], axis=2)
    first = dealt(first, "fs")
    second = dealt(second, "fs")

    chunks = []
    shifts = []
    shift_pieces = forget_shift[0].reshape(count, -1, rows)
    for step in range(count):
        chunk = tokens[0]
        shift = lax.dynamic_index_in_dim(shift_pieces, place ^ step, 0, False)
        if step:
            chunk = traded(chunk, "fs", step)
            shift = traded(shift, "fs", step)
        other = swapped(chunk)
        flat = jnp.concatenate(
            [jnp.where(side == 0, chunk, other), jnp.where(side == 0, other, chunk)], axis=1
        ).astype(jnp.float32)
        flat = flat * lax.rsqrt(jnp.mean(flat * flat, axis=-1, keepdims=True) + EPSILON)
        chunks.append((flat * norm_gain).astype(jnp.bfloat16))
        shifts.append(shift.T)
    normed = jnp.concatenate(chunks, axis=0)

    merge = lax.all_gather(merge_weight, "sp", axis=0)
    first = lax.all_gather(first, "sp", axis=0, tiled=True).reshape(2 * half, -1)
    second = lax.all_gather(second, "sp", axis=0, tiled=True).reshape(2 * half, -1)

    total = add_product(normed, first)
    width = query_weight.shape[1] // count
    queries = total[:, :width].astype(jnp.bfloat16)
    keys = total[:, width : 2 * width].astype(jnp.bfloat16)
    deep = value_weight.shape[1] // count
    values = total[:, 2 * width : 2 * width + deep].astype(jnp.bfloat16)
    gates = total[:, 2 * width + deep : total.shape[1] - spare]
    gate_apertures, cumulative, inputs = plane_states(
        keys,
        values,
        gates,
        own_part(forget_bias, 0, place, count),
        jnp.concatenate(shifts, axis=0),
        count,
    )

    others = add_product(normed, second).astype(jnp.bfloat16)
    channels = exit_weight.shape[1] // count
    outgates = others[:, :deep]
    exit_rows = others[:, deep : deep + channels]
    entry_rows = others[:, deep + channels : deep + 2 * channels]
    signal_rows = others[:, deep + 2 * channels :]
    mixed_in = (entry_rows.astype(jnp.float32) * signal_rows.astype(jnp.float32)).astype(
        jnp.bfloat16
    )
    mixed_in = mixed_in.reshape(count, rows, channels)
    rim = passed_along(mixed_in[:, rows - (KERNEL - 1) :], "sp", 1)
    padded = jnp.concatenate([rim, mixed_in], axis=1).astype(jnp.float32)
    taps = own_part(conv_kernel, 1, place, count)
    response = taps[0] * padded[:, 0:rows]
    for tap in range(1, KERNEL):
        response = response + taps[tap] * padded[:, tap : tap + rows]
    response = response.reshape(count * rows, channels)
    conv_out = (exit_rows.astype(jnp.float32) * response).astype(jnp.bfloat16)
    conv_other = swapped(conv_out)
    memory_out = memory_output(
        queries,
        keys,
        values,
        outgates,
        inputs,
        cumulative,
        gate_apertures,
        own_part(head_norm_gain, 0, place, count),
    )
    memory_other = swapped(memory_out)
    features = jnp.concatenate([memory_out, memory_other, conv_out, conv_other], axis=1)
    flipped = jnp.stack([merge[1], merge[0], merge[3], merge[2]])
    turned = jnp.where(side == 0, merge, flipped)
    turned = turned.reshape(-1, merge.shape[2])
    sent = []
    for step in range(count - 1, 0, -1):
        part = add_product(features[step * rows : (step + 1) * rows], turned)
        sent.append(traded(part.astype(jnp.bfloat16), "fs", step))
    mixed = add_product(features[:rows], turned)
    for part in sent:
        mixed = mixed + part.astype(jnp.float32)
    return mixed.astype(jnp.bfloat16)[None]


def local(*arguments):
    count = lax.axis_size("fs")
    merge_rows = arguments[14].shape[0]
    fits = (
        lax.axis_size("tp") == 2
        and lax.axis_size("sp") == 2 * lax.axis_size("tp")
        and count & (count - 1) == 0
        and arguments[7].shape[0] % count == 0
        and merge_rows == arguments[4].shape[1] // count
        and merge_rows == arguments[10].shape[1] // count
    )
    return by_plane(*arguments) if fits else by_position(*arguments)


def solution(mesh):
    placed = (
        P("fs", "sp", "tp"),
        P(),
        P(("sp", "fs"), "tp"),
        P(("sp", "fs"), "tp"),
        P(("sp", "fs"), "tp"),
        P(("sp", "fs"), "tp"),
        P(("sp", "fs"), None, "tp"),
        P("tp"),
        P("fs", "tp", "sp"),
        P("tp"),
        P(("sp", "fs"), "tp"),
        P(("sp", "fs"), "tp"),
        P(("sp", "fs"), "tp"),
        P(None, "tp"),
        P(("sp", "fs"), "tp"),
    )
    return jax.shard_map(
        local, mesh=mesh, in_specs=placed, out_specs=P("fs", "sp", "tp"), check_vma=False
    )
```
